32 devices in a mesh: sp: 4 (over x, core), dp: 8 (over z, y).
Axes of the slice: x: 2, y: 2, z: 4, core: 2. Of those that a mesh axis runs over, the one named last changes fastest.
Arguments:
- query: bfloat16 [8, 512, 1024], P('dp', None, 'sp'), may hold values from -120 to 120
- keys: bfloat16 [8, 512, 1024], P('dp', None, 'sp'), may hold values from -6 to 6
- values: bfloat16 [8, 512, 1024], P('dp', None, 'sp'), may hold values from -6 to 6
- output: bfloat16 [8, 512, 1024], P('dp'), may hold values from -1 to 1
- cum: float32 [8, 16, 512], P('dp', 'sp'), as said below
- d_out: bfloat16 [8, 512, 2048], P('dp', 'sp'), may hold values from -6 to 6
- w_out: bfloat16 [1024, 2048], P('dp'), may hold values from -0.125 to 0.125
Outputs:
- d_query: bfloat16 [8, 512, 1024], P('dp', 'sp')
- d_key: bfloat16 [8, 512, 1024], P('dp', 'sp')
- d_value: bfloat16 [8, 512, 1024], P('dp', 'sp')
- d_cum: float32 [8, 16, 512], P('dp', 'sp')
- d_w_out: float32 [1024, 2048], P('dp', 'sp')
The draws below stay inside these ranges and needn't reach their ends.
Inputs may be any that keep to these rules, and one draw needn't show every extreme that they name: cum never rises along positions.
All inputs are finite; a program needn't handle non-finite values.
Results may differ from the reference program's by a relative error of at most 0.008.
Values may be sent and summed in bfloat16 or wider, within the bound.
No kernel may reach another device: no remote copies, remote signals or barrier semaphores. Data moves between devices by JAX's collectives and lax.ppermute only.
A program may use at most 64 MiB of HBM per device.

```python
import jax
import jax.numpy as jnp
from jax import lax

D = 2048
HEAD_TOTAL = 16
HEAD = 64
TOK_DEV = 128
ATTN = 1024
SEQUENCE_LENGTH = 512
SEQUENCE_COUNT = 8


def shared_keys(key):
    return jnp.clip(jax.random.normal(jax.random.fold_in(key, 11), (SEQUENCE_COUNT, SEQUENCE_LENGTH, ATTN), jnp.float32), -6.0, 6.0)


def draw_keys(key, part):
    return shared_keys(key).astype(jnp.bfloat16)


def draw_query(key, part):
    base_query = jnp.clip(jax.random.normal(jax.random.fold_in(key, 12), (SEQUENCE_COUNT, SEQUENCE_LENGTH, ATTN), jnp.float32), -6.0, 6.0)
    return base_query.astype(jnp.bfloat16)


def draw_cum(key, part):
    shape = (SEQUENCE_COUNT, HEAD_TOTAL, SEQUENCE_LENGTH)
    slow_share = 0.5
    slow_heads = jax.random.uniform(jax.random.fold_in(key, 21), (SEQUENCE_COUNT, HEAD_TOTAL, 1)) < slow_share
    fast_rate = jnp.exp(jax.random.uniform(jax.random.fold_in(key, 22), (SEQUENCE_COUNT, HEAD_TOTAL, 1), jnp.float32, jnp.log(1.0 / 60.0), jnp.log(1.0 / 25.0)))
    slow_rate = 0.7 / SEQUENCE_LENGTH * jnp.exp(jax.random.uniform(jax.random.fold_in(key, 23), (SEQUENCE_COUNT, HEAD_TOTAL, 1), jnp.float32, -0.7, 0.7))
    blocks = SEQUENCE_LENGTH // TOK_DEV
    block_factor = jnp.exp(jax.random.uniform(jax.random.fold_in(key, 24), (SEQUENCE_COUNT, HEAD_TOTAL, blocks), jnp.float32, -0.7, 0.7))
    block_factor = jnp.repeat(block_factor, TOK_DEV, axis=2)
    roughness = jax.random.uniform(jax.random.fold_in(key, 25), shape, jnp.float32, 0.3, 1.7)
    decay_rates = jnp.where(slow_heads, slow_rate, fast_rate) * block_factor * roughness
    spike_positions = jax.random.randint(jax.random.fold_in(key, 26), (SEQUENCE_COUNT, HEAD_TOTAL, 3), 0, SEQUENCE_LENGTH)
    spike_length = jnp.log(1.0 - jax.random.uniform(jax.random.fold_in(key, 27), (SEQUENCE_COUNT, HEAD_TOTAL, 3), jnp.float32, 0.2, 0.5))
    locations = jnp.arange(SEQUENCE_LENGTH)
    spikes = jnp.sum(jnp.where(locations[None, None, None, :] == spike_positions[:, :, :, None], spike_length[:, :, :, None], 0.0), axis=2)
    return jnp.cumsum(spikes - decay_rates, axis=2)


def raised(result, key, source, target, shards_of, factor):
    owner, partner = [(jnp.arange(result.shape[dim]) // (result.shape[dim] // shards_of)).reshape([-1 if axis == dim else 1 for axis in range(result.ndim)]) for dim in (source, target)]
    chosen = jax.random.permutation(key, shards_of)[partner]
    strong = (owner == chosen) | (owner == (partner + shards_of // 2) % shards_of)
    return jnp.where(strong, factor * result, result)


def level_of(rng, dims, pieces, low, high):
    factor_of, own = 1.0, jax.random.fold_in(rng, 6)
    for axis_at, parts in pieces:
        steps = jnp.exp(jax.random.uniform(jax.random.fold_in(own, axis_at), (parts,), jnp.float32, low / len(pieces), high / len(pieces)))
        factor_of = factor_of * jnp.repeat(steps, dims[axis_at] // parts).reshape([-1 if axis == axis_at else 1 for axis in range(len(dims))])
    return factor_of


def gaussian(stream_key, shape, width, bound, cuts=(), kind=jnp.bfloat16):
    array = jax.random.normal(stream_key, shape, jnp.float32) * width
    if len(cuts) > 0:
        array = level_of(stream_key, shape, cuts, -0.22, 0.18) * array
    return jnp.clip(array, min=-bound, max=bound).astype(kind)


def heavy_noise(key, extent, spread, limit, pieces, heavy, kind=jnp.bfloat16):
    array = spread * jax.random.normal(key, extent, jnp.float32)
    if pieces:
        array = array * level_of(key, extent, pieces, -0.22, 0.18)
    return jnp.clip(raised(array, jax.random.fold_in(key, 3), *heavy), -limit, limit).astype(kind)


def setup_inputs(seed: int = 0) -> dict:
    seeds = jax.random.split(jax.random.key(seed), 8)
    query = draw_query(jax.random.fold_in(seeds[7], 71), 0)
    keys = draw_keys(jax.random.fold_in(seeds[7], 71), 0)
    values = gaussian(seeds[2], (SEQUENCE_COUNT, SEQUENCE_LENGTH, ATTN), 1.0, 6.0, ((0, 8), (2, 4)))
    output = heavy_noise(seeds[3], (SEQUENCE_COUNT, SEQUENCE_LENGTH, ATTN), 0.125, 1.0, ((0, 8),), (0, 2, 8, 2.0))
    cum = draw_cum(jax.random.fold_in(seeds[7], 71), 0)
    d_out = gaussian(seeds[5], (SEQUENCE_COUNT, SEQUENCE_LENGTH, D), 1.0, 6.0, ((0, 8), (1, 4)))
    w_out = gaussian(seeds[6], (ATTN, D), D ** -0.5, 0.125, ((0, 8),))
    return {"query": query, "keys": keys, "values": values, "output": output, "cum": cum, "d_out": d_out, "w_out": w_out}


def product(left, right, form):
    return jnp.einsum(form, left.astype(jnp.float32), right.astype(jnp.float32))


def head_grads(query, keys, values, output, cotangent, cum):
    head_count, length, head_width = query.shape
    span_rows = min(512, length)
    score_scale = head_width ** -0.5
    row_dots = jnp.sum(cotangent.astype(jnp.float32) * output.astype(jnp.float32), axis=2)
    positions = jnp.arange(length)

    def advance(totals, block_index):
        key_grad, value_grad, cum_grad = totals
        offset = (block_index * span_rows).astype(jnp.int32)
        query_blk = lax.dynamic_slice_in_dim(query, offset, span_rows, 1)
        cot_blk = lax.dynamic_slice_in_dim(cotangent, offset, span_rows, 1)
        cum_blk = lax.dynamic_slice_in_dim(cum, offset, span_rows, 1)
        dots_blk = lax.dynamic_slice_in_dim(row_dots, offset, span_rows, 1)
        scores = product(query_blk, keys, "hqe,hke->hqk") * score_scale
        scores = scores + cum_blk[:, :, None] - cum[:, None, :]
        query_pos = offset + jnp.arange(span_rows)
        causal = positions[None, :] <= query_pos[:, None]
        scores = jnp.where(causal[None], scores, -1e30)
        row_max = jnp.max(scores, axis=2, keepdims=True)
        weights = jnp.exp(scores - row_max)
        weights = weights / jnp.sum(weights, axis=2, keepdims=True)
        weights_b = weights.astype(jnp.bfloat16)
        d_prob = product(cot_blk, values, "hqe,hke->hqk")
        d_score = weights * (d_prob - dots_blk[:, :, None])
        score_b = d_score.astype(jnp.bfloat16)
        query_grad = (product(score_b, keys, "hqk,hke->hqe") * score_scale).astype(jnp.bfloat16)
        key_grad = key_grad + product(score_b, query_blk, "hqk,hqe->hke") * score_scale
        value_grad = value_grad + product(weights_b, cot_blk, "hqk,hqe->hke")
        cum_grad = cum_grad - jnp.sum(d_score, axis=1)
        own_part = lax.dynamic_slice_in_dim(cum_grad, offset, span_rows, 1) + jnp.sum(d_score, axis=2)
        cum_grad = lax.dynamic_update_slice_in_dim(cum_grad, own_part, offset, 1)
        return (key_grad, value_grad, cum_grad), query_grad

    start_state = (jnp.zeros(query.shape, jnp.float32), jnp.zeros(query.shape, jnp.float32),
                   jnp.zeros(cum.shape, jnp.float32))
    totals, query_blocks = lax.scan(advance, start_state, jnp.arange(length // span_rows))
    query_grad = jnp.transpose(query_blocks, (1, 0, 2, 3)).reshape(query.shape)
    return query_grad, totals[0].astype(jnp.bfloat16), totals[1].astype(jnp.bfloat16), totals[2]


def reference(query, keys, values, output, cum, d_out, w_out):
    def one_sequence(sequence):
        q_seq, k_seq, v_seq, o_seq, c_seq, g_seq = sequence
        d_attn = jnp.dot(g_seq, w_out.T, preferred_element_type=jnp.float32).astype(jnp.bfloat16)

        def heads_first(matrix):
            return jnp.transpose(matrix.reshape(SEQUENCE_LENGTH, HEAD_TOTAL, HEAD), (1, 0, 2))

        def tokens_first(matrix):
            return jnp.transpose(matrix, (1, 0, 2)).reshape(SEQUENCE_LENGTH, ATTN)

        grads = head_grads(heads_first(q_seq), heads_first(k_seq), heads_first(v_seq),
                           heads_first(o_seq), heads_first(d_attn), c_seq)
        return tokens_first(grads[0]), tokens_first(grads[1]), tokens_first(grads[2]), grads[3]

    d_query, d_key, d_value, d_cum = lax.map(one_sequence, (query, keys, values, output, cum, d_out))

    def accumulate(running, couple):
        return running + jnp.dot(couple[0].T, couple[1], preferred_element_type=jnp.float32), None

    d_w_out = lax.scan(accumulate, jnp.zeros((ATTN, D), jnp.float32), (output, d_out))[0]
    return d_query, d_key, d_value, d_cum, d_w_out
```

```python
import functools

import jax
import jax.numpy as jnp
from jax import lax
from jax.experimental import pallas as pl
from jax.experimental.pallas import tpu as pltpu
from jax.sharding import PartitionSpec as P

LANES = 128
F32 = jnp.float32
BF16 = jnp.bfloat16


def dot_nn(left, right):
    return lax.dot_general(left, right, (((1,), (0,)), ((), ())), preferred_element_type=F32)


def dot_nt(left, right):
    return lax.dot_general(left, right, (((1,), (1,)), ((), ())), preferred_element_type=F32)


def window(index, size):
    return pl.ds(pl.multiple_of(index * size, size), size)


def lane_head(value, head, width):
    lane = lax.broadcasted_iota(jnp.int32, value.shape, 1)
    inside = (lane >= head * width) & (lane < (head + 1) * width)
    return jnp.where(inside, value, jnp.zeros_like(value))


def row_head(value, head, width):
    row = lax.broadcasted_iota(jnp.int32, value.shape, 0)
    inside = (row >= head * width) & (row < (head + 1) * width)
    return jnp.where(inside, value, jnp.zeros_like(value))


def prob_kernel(heads, query_ref, keys_ref, output_ref, cum_ref, prob_ref, out_t_ref, keys_t_ref):
    length, width = query_ref.shape
    head_width = width // heads
    per_group = LANES // head_width
    scale = jnp.asarray(head_width**-0.5, BF16)
    cum = cum_ref[...]
    cum_cols = jnp.transpose(jnp.concatenate([cum] + [jnp.zeros_like(cum)] * (8 // heads - 1), 0))
    key_at = lax.broadcasted_iota(jnp.int32, (LANES, LANES), 0)
    query_at = lax.broadcasted_iota(jnp.int32, (LANES, LANES), 1)
    causal = key_at <= query_at
    for head in range(heads):
        lanes = pl.ds(head // per_group * LANES, LANES)
        keys_head = lane_head(keys_ref[:, lanes], head % per_group, head_width)
        cum_key = cum_cols[:, head : head + 1]
        for block in range(length // LANES):
            rows = (block + 1) * LANES
            own = pl.ds(block * LANES, LANES)
            scores = dot_nt(keys_head[:rows], query_ref[own, lanes] * scale)
            scores = scores + cum[head : head + 1, block * LANES : rows] - cum_key[:rows]
            last = jnp.where(causal, scores[block * LANES :], -1e30)
            scores = jnp.concatenate([scores[: block * LANES], last], 0) if block else last
            weights = jnp.exp(scores - jnp.max(scores, axis=0, keepdims=True))
            weights = weights * (1.0 / jnp.sum(weights, axis=0, keepdims=True))
            prob_ref[head, :rows, own] = weights.astype(BF16)
    out_t_ref[...] = jnp.transpose(output_ref[...])
    keys_t_ref[...] = jnp.transpose(keys_ref[...] * scale)


def weight_kernel(inner, *refs):
    out_t_ref, shards, (keep_ref, send_ref, columns_ref) = refs[0], refs[1:-3], refs[-3:]
    me, place = lax.axis_index("sp"), lax.axis_index("dp")
    outer, mine = place // inner, place % inner
    tokens = shards[0].shape[0]
    slots, block_rows, width = keep_ref.shape
    for step, shard in enumerate(shards):
        columns_ref[window(me ^ step, tokens), :] = shard[:, window(me, width)]
    columns = columns_ref[...]
    for slot in range(slots):
        target = (outer + slot) % slots
        keep = out_t_ref[window(target * inner + mine, block_rows), :]
        send = out_t_ref[window(target * inner + (mine ^ 1), block_rows), :]
        keep_ref[slot] = dot_nn(keep, columns)
        send_ref[slot] = dot_nn(send, columns).astype(BF16)


def merge_kernel(keep_ref, got_ref, own_ref, *send_refs):
    own_ref[...] = keep_ref[0] + got_ref[0].astype(F32)
    for slot, send_ref in enumerate(send_refs, 1):
        send_ref[...] = (keep_ref[slot] + got_ref[slot].astype(F32)).astype(BF16)


def finish_kernel(own_ref, *refs):
    total = own_ref[...]
    for got_ref in refs[:-1]:
        total = total + got_ref[...].astype(F32)
    refs[-1][...] = total


def grads_kernel(other, heads, steps, pieces, *refs):
    (prob_ref, query_ref, keys_t_ref, values_ref, out_t_ref), refs = refs[:5], refs[5:]
    shards, refs = refs[:steps], refs[steps:]
    weights, refs = refs[:pieces], refs[pieces:]
    slot_refs, refs = refs[:steps], refs[steps:]
    cum_ref, cot_ref, score_ref, query_grad_ref, key_grad_ref, value_grad_ref, sums_ref = refs
    me = lax.axis_index("sp")
    group = lax.axis_index("dp") % 2
    if other:
        group = 1 - group
    length, width = query_ref.shape
    head_width = width // heads
    per_group = LANES // head_width
    tokens = shards[0].shape[0]
    scale = jnp.asarray(head_width**-0.5, BF16)
    weight = jnp.concatenate([piece[...] for piece in weights], 0)
    for step, shard in enumerate(shards):
        cot_ref[:, window(me ^ step, tokens)] = dot_nt(weight, shard[...]).astype(BF16)
    lanes = window(group, LANES)
    cot = cot_ref[...]
    query = query_ref[:, lanes] * scale
    keys_t = keys_t_ref[lanes, :]
    out_t = out_t_ref[window(me * (width // LANES) + group, LANES), :]
    product = cot.astype(F32) * out_t.astype(F32)
    blocks = length // LANES
    key_grads, value_grads = [0.0] * blocks, [0.0] * blocks
    query_grads = [0.0] * blocks
    sum_columns, sum_rows = [], []
    for head in range(per_group):
        index = group * per_group + head
        cot_head = row_head(cot, head, head_width)
        query_head = lane_head(query, head, head_width)
        keys_head = row_head(keys_t, head, head_width)
        dots = jnp.sum(product[head * head_width : (head + 1) * head_width], axis=0, keepdims=True)
        rows_sum = []
        for block in range(blocks):
            rows = (block + 1) * LANES
            own = pl.ds(block * LANES, LANES)
            at = slice(block * LANES, rows)
            d_prob = dot_nn(values_ref[:rows, lanes], cot_head[:, at])
            d_score = prob_ref[index, :rows, own].astype(F32) * (d_prob - dots[:, at])
            rows_sum.append(jnp.sum(d_score, axis=0, keepdims=True))
            if block:
                sums_ref[: block * LANES, :] += d_score[: block * LANES]
            sums_ref[own, :] = d_score[block * LANES :]
            rounded = d_score.astype(BF16)
            score_ref[:rows, own] = rounded
            query_grads[block] += dot_nn(keys_head[:, :rows], rounded)
        for block in range(blocks):
            own = pl.ds(block * LANES, LANES)
            start = block * LANES
            key_grads[block] += dot_nn(score_ref[own, start:], query_head[start:])
            value_grads[block] += dot_nt(prob_ref[index, own, start:], cot_head[:, start:])
        sum_columns.append(jnp.sum(sums_ref[...], axis=1, keepdims=True))
        sum_rows.append(jnp.concatenate(rows_sum, 1))
    lane = lax.broadcasted_iota(jnp.int32, (length, LANES), 1)
    spread = jnp.zeros((length, LANES), F32)
    for head in range(per_group):
        spread = jnp.where(lane == head, sum_columns[head], spread)
    cum_ref[...] = jnp.concatenate(sum_rows, 0) - jnp.transpose(spread)[:per_group]
    for block in range(blocks):
        own = pl.ds(block * LANES, LANES)
        query_grad_ref[own, :] = jnp.transpose(query_grads[block]).astype(BF16)
        key_grad_ref[own, :] = key_grads[block].astype(BF16)
        value_grad_ref[own, :] = value_grads[block].astype(BF16)
    for step, slot_ref in enumerate(slot_refs):
        here = window(me ^ step, tokens)
        slot_ref[0] = query_grad_ref[here, :]
        slot_ref[1] = key_grad_ref[here, :]
        slot_ref[2] = value_grad_ref[here, :]


def place_kernel(steps, *refs):
    first, second = refs[:steps], refs[steps : 2 * steps]
    first_cum_ref, second_cum_ref = refs[2 * steps : 2 * steps + 2]
    grad_refs, cum_ref = refs[2 * steps + 2 : -1], refs[-1]
    me, mine = lax.axis_index("sp"), lax.axis_index("dp") % 2
    for step in range(steps):
        for group, parts in ((mine, first), (1 - mine, second)):
            columns = window((me ^ step) * 2 + group, LANES)
            for kind, grad_ref in enumerate(grad_refs):
                grad_ref[:, columns] = parts[step][kind]
    low, high = first_cum_ref[...], second_cum_ref[...]
    swap = jnp.full(low.shape, mine, jnp.int32) == 1
    cum_ref[...] = jnp.concatenate(
        [jnp.where(swap, high, low), jnp.where(swap, low, high)], 0
    )


def call(kernel, outs, args, scratch=()):
    return pl.pallas_call(
        kernel,
        out_shape=[jax.ShapeDtypeStruct(shape, kind) for shape, kind in outs],
        in_specs=[pl.BlockSpec(memory_space=pltpu.VMEM)] * len(args),
        out_specs=[pl.BlockSpec(memory_space=pltpu.VMEM)] * len(outs),
        scratch_shapes=[pltpu.VMEM(shape, kind) for shape, kind in scratch],
    )(*args)


def fused_shards(sizes, query, keys, values, output, cum, d_out, w_out):
    split, groups = sizes
    inner = groups // split
    query, keys, values, output, cum, d_out = (
        query[0], keys[0], values[0], output[0], cum[0], d_out[0]
    )
    length, width = query.shape
    heads = cum.shape[0]
    head_width = width // heads
    per_group = LANES // head_width
    tokens, model = d_out.shape
    block_rows = w_out.shape[0]
    attn = output.shape[1]
    piece_rows = block_rows // split

    def device(shard, group):
        return shard * groups + group

    def sp_swap(array, step):
        return lax.ppermute(array, "sp", [(i, i ^ step) for i in range(split)])

    def inner_swap(array):
        return lax.ppermute(array, "dp", [(i, i ^ 1) for i in range(groups)])

    def outer_shift(array, step):
        pairs = []
        for outer in range(split):
            for at in range(inner):
                pairs.append((outer * inner + at, (outer + step) % split * inner + at))
        return lax.ppermute(array, "dp", pairs)

    first_rows = []
    for step in range(split):
        pairs = []
        for shard in range(split):
            for at in range(inner):
                for replica in range(split):
                    source = device(replica, shard * inner + at)
                    pairs.append((source, device(shard, (replica + step) % split * inner + at)))
        piece = w_out[step * piece_rows : (step + 1) * piece_rows]
        first_rows.append(lax.ppermute(piece, ("sp", "dp"), pairs))

    far = sp_swap(d_out, 2)
    shards = [d_out, sp_swap(d_out, 1), far, sp_swap(far, 1)]

    second_rows = [inner_swap(piece) for piece in first_rows]

    prob, out_t, keys_t = call(
        functools.partial(prob_kernel, heads),
        [((heads, length, length), BF16), ((attn, length), BF16), ((width, length), BF16)],
        (query, keys, output, cum),
    )
    share = (split, block_rows, model // split)
    keep, send = call(
        functools.partial(weight_kernel, inner),
        [(share, F32), (share, BF16)],
        (out_t, *shards),
        [((length, model // split), BF16)],
    )
    got = inner_swap(send)
    own, *parts = call(
        merge_kernel, [(share[1:], F32)] + [(share[1:], BF16)] * (split - 1), (keep, got)
    )
    parts = [outer_shift(part, step) for step, part in enumerate(parts, 1)]
    grad_weight, = call(finish_kernel, [(share[1:], F32)], (own, *parts))

    slot = (3, tokens, LANES)
    arrived, cums = [], []
    for other, rows in ((False, first_rows), (True, second_rows)):
        *slots, part_cum = call(
            functools.partial(grads_kernel, other, heads, split, split),
            [(slot, BF16)] * split + [((per_group, length), F32)],
            (prob, query, keys_t, values, out_t, *shards, *rows),
            [
                ((LANES, length), BF16),
                ((length, length), BF16),
                ((length, LANES), BF16),
                ((length, LANES), BF16),
                ((length, LANES), BF16),
                ((length, LANES), F32),
            ],
        )
        arrived.append([slots[0]] + [sp_swap(slots[i], i) for i in range(1, split)])
        cums.append(part_cum)
    query_grad, key_grad, value_grad, cum_grad = call(
        functools.partial(place_kernel, split),
        [((tokens, attn), BF16)] * 3 + [((heads, length), F32)],
        (*arrived[0], *arrived[1], *cums),
    )
    return query_grad[None], key_grad[None], value_grad[None], cum_grad[None], grad_weight


def head_grads(query, keys, values, output, cotangent, cum):
    head_count, length, head_width = query.shape
    span_rows = min(512, length)
    score_scale = head_width ** (-0.5)
    row_dots = jnp.sum(cotangent.astype(jnp.float32) * output.astype(jnp.float32), axis=2)
    positions = jnp.arange(length)

    def product(left, right, form):
        return jnp.einsum(form, left, right, preferred_element_type=jnp.float32)

    def advance(totals, block_index):
        key_grad, value_grad, cum_grad = totals
        offset = block_index * span_rows
        query_blk = lax.dynamic_slice_in_dim(query, offset, span_rows, 1)
        cot_blk = lax.dynamic_slice_in_dim(cotangent, offset, span_rows, 1)
        cum_blk = lax.dynamic_slice_in_dim(cum, offset, span_rows, 1)
        dots_blk = lax.dynamic_slice_in_dim(row_dots, offset, span_rows, 1)
        scores = product(query_blk, keys, "hqe,hke->hqk") * score_scale
        scores = scores + cum_blk[:, :, None] - cum[:, None, :]
        query_pos = offset + jnp.arange(span_rows)
        causal = positions[None, :] <= query_pos[:, None]
        scores = jnp.where(causal[None], scores, -1e30)
        row_max = jnp.max(scores, axis=2, keepdims=True)
        weights = jnp.exp(scores - row_max)
        weights = weights / jnp.sum(weights, axis=2, keepdims=True)
        weights_b = weights.astype(jnp.bfloat16)
        d_prob = product(cot_blk, values, "hqe,hke->hqk")
        d_score = weights * (d_prob - dots_blk[:, :, None])
        score_b = d_score.astype(jnp.bfloat16)
        query_grad = (product(score_b, keys, "hqk,hke->hqe") * score_scale).astype(jnp.bfloat16)
        key_grad = key_grad + product(score_b, query_blk, "hqk,hqe->hke") * score_scale
        value_grad = value_grad + product(weights_b, cot_blk, "hqk,hqe->hke")
        cum_grad = cum_grad - jnp.sum(d_score, axis=1)
        own_part = lax.dynamic_slice_in_dim(cum_grad, offset, span_rows, 1) + jnp.sum(
            d_score, axis=2
        )
        cum_grad = lax.dynamic_update_slice_in_dim(cum_grad, own_part, offset, 1)
        return ((key_grad, value_grad, cum_grad), query_grad)

    start_state = (
        jnp.zeros(query.shape, jnp.float32),
        jnp.zeros(query.shape, jnp.float32),
        jnp.zeros(cum.shape, jnp.float32),
    )
    totals, query_blocks = lax.scan(advance, start_state, jnp.arange(length // span_rows))
    query_grad = jnp.transpose(query_blocks, (1, 0, 2, 3)).reshape(query.shape)
    return (query_grad, totals[0].astype(jnp.bfloat16), totals[1].astype(jnp.bfloat16), totals[2])


def shards(query, keys, values, output, cum, d_out, w_out):
    local_rows = d_out[0]
    whole_output = output[0]
    d_attn = lax.dot_general(
        local_rows,
        lax.all_gather(w_out, "dp", axis=0, tiled=True),
        (((1,), (1,)), ((), ())),
        preferred_element_type=jnp.float32,
    ).astype(jnp.bfloat16)
    head_cot, column_part = (
        lax.all_to_all(d_attn[None], "sp", split_axis=2, concat_axis=1, tiled=True),
        lax.all_to_all(d_out, "sp", split_axis=2, concat_axis=1, tiled=True),
    )
    grad_weight = lax.psum_scatter(
        lax.dot_general(
            whole_output,
            column_part[0],
            (((0,), (0,)), ((), ())),
            preferred_element_type=jnp.float32,
        ),
        "dp",
        scatter_dimension=0,
        tiled=True,
    )
    head_cols = query.shape[2]
    head_count = cum.shape[1]
    head_width = head_cols // head_count
    seq_length = query.shape[1]
    own_output = lax.dynamic_slice_in_dim(
        whole_output, lax.axis_index("sp") * head_cols, head_cols, 1
    )

    def heads_first(matrix):
        return jnp.transpose(matrix.reshape(seq_length, head_count, head_width), (1, 0, 2))

    def tokens_first(matrix):
        return jnp.transpose(matrix, (1, 0, 2)).reshape(1, seq_length, head_cols)

    grads = head_grads(
        heads_first(query[0]),
        heads_first(keys[0]),
        heads_first(values[0]),
        heads_first(own_output),
        heads_first(head_cot[0]),
        cum[0],
    )
    query_grad, key_grad, value_grad = (
        lax.all_to_all(tokens_first(grads[0]), "sp", split_axis=1, concat_axis=2, tiled=True),
        lax.all_to_all(tokens_first(grads[1]), "sp", split_axis=1, concat_axis=2, tiled=True),
        lax.all_to_all(tokens_first(grads[2]), "sp", split_axis=1, concat_axis=2, tiled=True),
    )
    return (query_grad, key_grad, value_grad, grads[3][None], grad_weight)


def fits(sizes, args):
    split, groups = sizes
    query, output, cum, d_out, w_out = args[0], args[3], args[4], args[5], args[6]
    length, attn = query.shape[1:]
    width, heads = attn // split, cum.shape[1] // split
    head_width = width // max(heads, 1)
    return (
        split == 4
        and groups == 2 * split
        and width == 2 * LANES
        and heads * head_width == width
        and LANES % head_width == 0
        and 8 % heads == 0
        and head_width**0.5 % 1 == 0
        and head_width & (head_width - 1) == 0
        and w_out.shape[0] // groups == LANES
        and output.shape[2] == attn
        and d_out.shape[1] // split == LANES
        and d_out.shape[2] % (split * LANES) == 0
    )


def solution(mesh):
    placed = (
        P("dp", None, "sp"),
        P("dp", None, "sp"),
        P("dp", None, "sp"),
        P("dp", None, None),
        P("dp", "sp", None),
        P("dp", "sp", None),
        P("dp", None),
    )
    sizes = (mesh.shape["sp"], mesh.shape["dp"])

    def step(*args):
        body = functools.partial(fused_shards, sizes) if fits(sizes, args) else shards
        return jax.shard_map(
            body,
            mesh=mesh,
            in_specs=placed,
            out_specs=(
                P("dp", "sp", None),
                P("dp", "sp", None),
                P("dp", "sp", None),
                P("dp", "sp", None),
                P("dp", "sp"),
            ),
            check_vma=False,
        )(*args)

    return step
```

```python
import functools

import jax
import jax.numpy as jnp
from jax import lax
from jax.experimental import pallas as pl
from jax.experimental.pallas import tpu as pltpu
from jax.sharding import PartitionSpec as P


LANES = 128
F32 = jnp.float32
BF16 = jnp.bfloat16
KERNEL_BYTES = 16 << 20


def dot_nn(left, right):
    return lax.dot_general(left, right, (((1,), (0,)), ((), ())), preferred_element_type=F32)


def dot_nt(left, right):
    return lax.dot_general(left, right, (((1,), (1,)), ((), ())), preferred_element_type=F32)


def window(index, size):
    return pl.ds(pl.multiple_of(index * size, size), size)


def lane_head(value, head, width):
    lane = lax.broadcasted_iota(jnp.int32, value.shape, 1)
    inside = (lane >= head * width) & (lane < (head + 1) * width)
    return jnp.where(inside, value, jnp.zeros_like(value))


def row_head(value, head, width):
    row = lax.broadcasted_iota(jnp.int32, value.shape, 0)
    inside = (row >= head * width) & (row < (head + 1) * width)
    return jnp.where(inside, value, jnp.zeros_like(value))


def prep_kernel(halves, d_out_hbm, w_out_hbm, *refs):
    parts, sems = refs[:-1], refs[-1]
    width = parts[0].shape[1]
    rows = parts[2].shape[0]
    chip = lax.axis_index("sp") // 2
    sources = [d_out_hbm.at[:, window(1 - chip, width)], d_out_hbm.at[:, window(chip, width)]]
    sources += [w_out_hbm.at[pl.ds(half * rows, rows), :] for half in range(halves)]
    copies = []
    for index, (source, part) in enumerate(zip(sources, parts)):
        copies.append(pltpu.make_async_copy(source, part, sems.at[index]))
        copies[-1].start()
    for copy in copies:
        copy.wait()


def prob_kernel(heads, query_hbm, keys_hbm, output_hbm, cum_hbm, *refs):
    prob_ref, out_t_ref, keys_t_ref, query_ref, keys_ref, output_ref, cum_ref, sems = refs
    copies = []
    for index, (source, part) in enumerate(
        (
            (cum_hbm, cum_ref),
            (query_hbm, query_ref),
            (keys_hbm, keys_ref),
            (output_hbm, output_ref),
        )
    ):
        copies.append(pltpu.make_async_copy(source, part, sems.at[index]))
        copies[-1].start()
    for copy in copies[:3]:
        copy.wait()
    length, width = query_ref.shape
    head_width = width // heads
    per_group = LANES // head_width
    scale = jnp.asarray(head_width**-0.5, BF16)
    cum = cum_ref[...]
    cum_cols = jnp.transpose(jnp.concatenate([cum] + [jnp.zeros_like(cum)] * (8 // heads - 1), 0))
    key_at = lax.broadcasted_iota(jnp.int32, (LANES, LANES), 0)
    query_at = lax.broadcasted_iota(jnp.int32, (LANES, LANES), 1)
    causal = key_at <= query_at
    for head in range(heads):
        lanes = pl.ds(head // per_group * LANES, LANES)
        keys_head = lane_head(keys_ref[:, lanes], head % per_group, head_width)
        cum_key = cum_cols[:, head : head + 1]
        for block in range(length // LANES):
            rows = (block + 1) * LANES
            own = pl.ds(block * LANES, LANES)
            scores = dot_nt(keys_head[:rows], query_ref[own, lanes] * scale)
            scores = scores + cum[head : head + 1, block * LANES : rows] - cum_key[:rows]
            last = jnp.where(causal, scores[block * LANES :], -1e30)
            scores = jnp.concatenate([scores[: block * LANES], last], 0) if block else last
            weights = jnp.exp(scores - jnp.max(scores, axis=0, keepdims=True))
            weights = weights * (1.0 / jnp.sum(weights, axis=0, keepdims=True))
            prob_ref[head, :rows, own] = weights.astype(BF16)
    keys_t_ref[...] = jnp.transpose(keys_ref[...] * scale)
    copies[3].wait()
    out_t_ref[...] = jnp.transpose(output_ref[...])


def weight_kernel(inner, out_t_ref, own_ref, near_ref, far_ref, cross_ref, *refs):
    keep_ref, give_ref, stay_ref, *send_refs, columns_ref = refs
    me, place = lax.axis_index("sp"), lax.axis_index("dp")
    outer, mine = place // inner, place % inner
    tokens = own_ref.shape[0]
    half = keep_ref.shape[2]
    block_rows = keep_ref.shape[1]
    for step, (shard, at) in enumerate(
        ((own_ref, me % 2), (near_ref, me), (far_ref, me % 2), (cross_ref, me % 2))
    ):
        columns_ref[window(me ^ step, tokens), :] = shard[:, window(at, 2 * half)]
    columns = columns_ref[...]
    for step, to_ref in enumerate((stay_ref, *send_refs)):
        for index, by_inner in enumerate((keep_ref, give_ref)):
            block = (outer ^ step) * inner + (mine ^ index)
            part = dot_nn(out_t_ref[window(block, block_rows), :], columns)
            by_inner[step] = part[:, :half].astype(by_inner.dtype)
            to_ref[index] = part[:, half:].astype(to_ref.dtype)


def outer_merge_kernel(stay_ref, *refs):
    got_refs, (own_ref, send_ref) = refs[:-2], refs[-2:]
    total = stay_ref[...]
    for got_ref in got_refs:
        total = total + got_ref[...].astype(F32)
    own_ref[...] = total[0]
    send_ref[...] = total[1].astype(BF16)


def inner_merge_kernel(keep_ref, got_ref, own_ref, *send_refs):
    total = keep_ref[...] + got_ref[...].astype(F32)
    own_ref[...] = total[0]
    for step, send_ref in enumerate(send_refs, 1):
        send_ref[...] = total[step].astype(BF16)


def finish_kernel(first_ref, second_ref, last_ref, *refs):
    got_refs, total_ref = refs[:-1], refs[-1]
    first = first_ref[...]
    half = first.shape[1]
    for got_ref in got_refs:
        first = first + got_ref[...].astype(F32)
    total_ref[:, :half] = first
    total_ref[:, half:] = second_ref[...] + last_ref[...].astype(F32)


def grads_kernel(other, heads, steps, pieces, *refs):
    (prob_ref, query_ref, keys_t_ref, values_ref, out_t_ref), refs = refs[:5], refs[5:]
    near_ref, refs = refs[0], refs[1:]
    parted, refs = ((0, refs[:2]), (2, refs[2:4]), (3, refs[4:6])), refs[6:]
    weights, refs = refs[:pieces], refs[pieces:]
    before = ()
    if other:
        before, refs = refs[:steps], refs[steps:]
    slot_refs, refs = refs[:steps], refs[steps:]
    cum_ref, cot_ref, score_ref, query_grad_ref, key_grad_ref, value_grad_ref, sums_ref = refs[:7]
    weight_ref = refs[7]
    me = lax.axis_index("sp")
    group = lax.axis_index("dp") % 2
    if other:
        group = 1 - group
    length, width = query_ref.shape
    head_width = width // heads
    per_group = LANES // head_width
    tokens = near_ref.shape[0]
    scale = jnp.asarray(head_width**-0.5, BF16)
    piece_rows = LANES // pieces
    for index, piece in enumerate(weights):
        weight_ref[pl.ds(index * piece_rows, piece_rows), :] = piece[...]
    cot_ref[:, window(me ^ 1, tokens)] = dot_nt(weight_ref[...], near_ref[...]).astype(BF16)
    for step, (here, there) in parted:
        half = here.shape[1]
        cot = dot_nt(weight_ref[:, window(me // 2, half)], here[...])
        cot = cot + dot_nt(weight_ref[:, window(1 - me // 2, half)], there[...])
        cot_ref[:, window(me ^ step, tokens)] = cot.astype(BF16)
    lanes = window(group, LANES)
    cot = cot_ref[...]
    query = query_ref[:, lanes] * scale
    keys_t = keys_t_ref[lanes, :]
    out_t = out_t_ref[window(me * (width // LANES) + group, LANES), :]
    product = cot.astype(F32) * out_t.astype(F32)
    blocks = length // LANES
    key_grads, value_grads = [0.0] * blocks, [0.0] * blocks
    query_grads = [0.0] * blocks
    sum_columns, sum_rows = [], []
    for head in range(per_group):
        index = group * per_group + head
        cot_head = row_head(cot, head, head_width)
        query_head = lane_head(query, head, head_width)
        keys_head = row_head(keys_t, head, head_width)
        dots = jnp.sum(product[head * head_width : (head + 1) * head_width], axis=0, keepdims=True)
        rows_sum = []
        for block in range(blocks):
            rows = (block + 1) * LANES
            own = pl.ds(block * LANES, LANES)
            at = slice(block * LANES, rows)
            d_prob = dot_nn(values_ref[:rows, lanes], cot_head[:, at])
            d_score = prob_ref[index, :rows, own].astype(F32) * (d_prob - dots[:, at])
            rows_sum.append(jnp.sum(d_score, axis=0, keepdims=True))
            if block:
                sums_ref[: block * LANES, :] += d_score[: block * LANES]
            sums_ref[own, :] = d_score[block * LANES :]
            rounded = d_score.astype(BF16)
            score_ref[:rows, own] = rounded
            query_grads[block] += dot_nn(keys_head[:, :rows], rounded)
        for block in range(blocks):
            own = pl.ds(block * LANES, LANES)
            start = block * LANES
            key_grads[block] += dot_nn(score_ref[own, start:], query_head[start:])
            value_grads[block] += dot_nt(prob_ref[index, own, start:], cot_head[:, start:])
        sum_columns.append(jnp.sum(sums_ref[...], axis=1, keepdims=True))
        sum_rows.append(jnp.concatenate(rows_sum, 1))
    lane = lax.broadcasted_iota(jnp.int32, (length, LANES), 1)
    spread = jnp.zeros((length, LANES), F32)
    for head in range(per_group):
        spread = jnp.where(lane == head, sum_columns[head], spread)
    cum_ref[...] = jnp.concatenate(sum_rows, 0) - jnp.transpose(spread)[:per_group]
    for block in range(blocks):
        own = pl.ds(block * LANES, LANES)
        query_grad_ref[own, :] = jnp.transpose(query_grads[block]).astype(BF16)
        key_grad_ref[own, :] = key_grads[block].astype(BF16)
        value_grad_ref[own, :] = value_grads[block].astype(BF16)
    kinds = 3
    for step, slot_ref in enumerate(slot_refs):
        here = window(me ^ step, tokens)
        if other:
            slot_ref[:kinds] = before[step][...]
        start = kinds if other else 0
        slot_ref[start] = query_grad_ref[here, :]
        slot_ref[start + 1] = key_grad_ref[here, :]
        slot_ref[start + 2] = value_grad_ref[here, :]


def place_kernel(*refs):
    parts, (first_cum_ref, second_cum_ref) = refs[:-6], refs[-6:-4]
    grad_refs, cum_ref = refs[-4:-1], refs[-1]
    me, mine = lax.axis_index("sp"), lax.axis_index("dp") % 2
    for step, part in enumerate(parts):
        for index, group in enumerate((mine, 1 - mine)):
            columns = window((me ^ step) * 2 + group, LANES)
            for kind, grad_ref in enumerate(grad_refs):
                grad_ref[:, columns] = part[index * len(grad_refs) + kind]
    low, high = first_cum_ref[...], second_cum_ref[...]
    swap = jnp.full(low.shape, mine, jnp.int32) == 1
    cum_ref[...] = jnp.concatenate(
        [jnp.where(swap, high, low), jnp.where(swap, low, high)], 0
    )


def call(kernel, outs, args, scratch=(), inputs=pltpu.VMEM, copies=0):
    scratch_shapes = [pltpu.VMEM(shape, kind) for shape, kind in scratch]
    if copies:
        scratch_shapes.append(pltpu.SemaphoreType.DMA((copies,)))
    run = pl.pallas_call(
        kernel,
        out_shape=[jax.ShapeDtypeStruct(shape, kind) for shape, kind in outs],
        in_specs=[pl.BlockSpec(memory_space=inputs)] * len(args),
        out_specs=[pl.BlockSpec(memory_space=pltpu.VMEM)] * len(outs),
        scratch_shapes=scratch_shapes,
        compiler_params=pltpu.CompilerParams(vmem_limit_bytes=KERNEL_BYTES),
    )
    if inputs is pltpu.HBM:
        args = [pltpu.with_memory_space_constraint(array, inputs) for array in args]
    return run(*args)


def fused_shards(sizes, query, keys, values, output, cum, d_out, w_out):
    split, groups = sizes
    inner = groups // split
    query, keys, values, output, cum, d_out = (
        query[0], keys[0], values[0], output[0], cum[0], d_out[0]
    )
    length, width = query.shape
    heads = cum.shape[0]
    head_width = width // heads
    per_group = LANES // head_width
    tokens, model = d_out.shape
    block_rows = w_out.shape[0]
    attn = output.shape[1]

    def device(shard, group):
        return shard * groups + group

    def sp_swap(array, step):
        return lax.ppermute(array, "sp", [(i, i ^ step) for i in range(split)])

    def inner_swap(array):
        return lax.ppermute(array, "dp", [(i, i ^ 1) for i in range(groups)])

    def outer_swap(array, step):
        pairs = []
        for outer in range(split):
            for at in range(inner):
                pairs.append((outer * inner + at, (outer ^ step) * inner + at))
        return lax.ppermute(array, "dp", pairs)

    def spread(replica, half):
        return (replica + half) % split

    halves = split
    half_rows = block_rows // halves
    away, home, *cuts = call(
        functools.partial(prep_kernel, halves),
        [((tokens, model // 2), BF16)] * 2 + [((half_rows, model), BF16)] * halves,
        (d_out, w_out),
        inputs=pltpu.HBM,
        copies=2 + halves,
    )
    first_rows = []
    for half in range(halves):
        pairs = []
        for shard in range(split):
            for at in range(inner):
                for replica in range(split):
                    source = device(replica, shard * inner + at)
                    pairs.append((source, device(shard, spread(replica, half) * inner + at)))
        first_rows.append(lax.ppermute(cuts[half], ("sp", "dp"), pairs))
    second_rows = [inner_swap(piece) for piece in first_rows]

    near = sp_swap(d_out, 1)
    far_here = sp_swap(away, 2)
    far_there = sp_swap(home, 2)
    cross_here = sp_swap(far_here, 1)
    cross_there = sp_swap(far_there, 1)

    prob, out_t, keys_t = call(
        functools.partial(prob_kernel, heads),
        [((heads, length, length), BF16), ((attn, length), BF16), ((width, length), BF16)],
        (query, keys, output, cum),
        [((length, width), BF16)] * 2 + [((length, attn), BF16), ((heads, length), F32)],
        inputs=pltpu.HBM,
        copies=4,
    )
    half = model // split // 2
    share = (block_rows, half)
    keep, give, stay, *parts = call(
        functools.partial(weight_kernel, inner),
        [((split, *share), F32), ((split, *share), BF16), ((inner, *share), F32)]
        + [((inner, *share), BF16)] * (split - 1),
        (out_t, home, near, far_here, cross_here),
        [((length, 2 * half), BF16)],
    )
    parts = [outer_swap(part, step) for step, part in enumerate(parts, 1)]
    second, last = call(outer_merge_kernel, [(share, F32), (share, BF16)], (stay, *parts))
    last = inner_swap(last)
    first, *parts = call(
        inner_merge_kernel, [(share, F32)] + [(share, BF16)] * (split - 1), (keep, inner_swap(give))
    )
    parts = [outer_swap(part, step) for step, part in enumerate(parts, 1)]
    grad_weight, = call(
        finish_kernel, [((block_rows, 2 * half), F32)], (first, second, last, *parts)
    )

    slots, cums = [], []
    for other, rows in ((False, first_rows), (True, second_rows)):
        kinds = 6 if other else 3
        *slots, part_cum = call(
            functools.partial(grads_kernel, other, heads, split, halves),
            [((kinds, tokens, LANES), BF16)] * split + [((per_group, length), F32)],
            (
                prob, query, keys_t, values, out_t, near,
                home, away, far_here, far_there, cross_here, cross_there, *rows, *slots,
            ),
            [
                ((LANES, length), BF16),
                ((length, length), BF16),
                ((length, LANES), BF16),
                ((length, LANES), BF16),
                ((length, LANES), BF16),
                ((length, LANES), F32),
                ((LANES, model), BF16),
            ],
        )
        cums.append(part_cum)
    arrived = [slots[0]] + [sp_swap(slots[i], i) for i in range(1, split)]
    query_grad, key_grad, value_grad, cum_grad = call(
        place_kernel, [((tokens, attn), BF16)] * 3 + [((heads, length), F32)], (*arrived, *cums)
    )
    return query_grad[None], key_grad[None], value_grad[None], cum_grad[None], grad_weight


def head_grads(query, keys, values, output, cotangent, cum):
    _, length, head_width = query.shape
    span_rows = min(512, length)
    score_scale = head_width ** (-0.5)
    row_dots = jnp.sum(cotangent.astype(jnp.float32) * output.astype(jnp.float32), axis=2)
    positions = jnp.arange(length)

    def product(left, right, form):
        return jnp.einsum(form, left, right, preferred_element_type=jnp.float32)

    def advance(totals, block_index):
        key_grad, value_grad, cum_grad = totals
        offset = block_index * span_rows
        query_blk = lax.dynamic_slice_in_dim(query, offset, span_rows, 1)
        cot_blk = lax.dynamic_slice_in_dim(cotangent, offset, span_rows, 1)
        cum_blk = lax.dynamic_slice_in_dim(cum, offset, span_rows, 1)
        dots_blk = lax.dynamic_slice_in_dim(row_dots, offset, span_rows, 1)
        scores = product(query_blk, keys, "hqe,hke->hqk") * score_scale
        scores = scores + cum_blk[:, :, None] - cum[:, None, :]
        query_pos = offset + jnp.arange(span_rows)
        causal = positions[None, :] <= query_pos[:, None]
        scores = jnp.where(causal[None], scores, -1e30)
        row_max = jnp.max(scores, axis=2, keepdims=True)
        weights = jnp.exp(scores - row_max)
        weights = weights / jnp.sum(weights, axis=2, keepdims=True)
        weights_b = weights.astype(jnp.bfloat16)
        d_prob = product(cot_blk, values, "hqe,hke->hqk")
        d_score = weights * (d_prob - dots_blk[:, :, None])
        score_b = d_score.astype(jnp.bfloat16)
        query_grad = (product(score_b, keys, "hqk,hke->hqe") * score_scale).astype(jnp.bfloat16)
        key_grad = key_grad + product(score_b, query_blk, "hqk,hqe->hke") * score_scale
        value_grad = value_grad + product(weights_b, cot_blk, "hqk,hqe->hke")
        cum_grad = cum_grad - jnp.sum(d_score, axis=1)
        own_part = lax.dynamic_slice_in_dim(cum_grad, offset, span_rows, 1) + jnp.sum(
            d_score, axis=2
        )
        cum_grad = lax.dynamic_update_slice_in_dim(cum_grad, own_part, offset, 1)
        return ((key_grad, value_grad, cum_grad), query_grad)

    start_state = (
        jnp.zeros(query.shape, jnp.float32),
        jnp.zeros(query.shape, jnp.float32),
        jnp.zeros(cum.shape, jnp.float32),
    )
    totals, query_blocks = lax.scan(advance, start_state, jnp.arange(length // span_rows))
    query_grad = jnp.transpose(query_blocks, (1, 0, 2, 3)).reshape(query.shape)
    return (query_grad, totals[0].astype(jnp.bfloat16), totals[1].astype(jnp.bfloat16), totals[2])


def shards(query, keys, values, output, cum, d_out, w_out):
    local_rows = d_out[0]
    whole_output = output[0]
    d_attn = lax.dot_general(
        local_rows,
        lax.all_gather(w_out, "dp", axis=0, tiled=True),
        (((1,), (1,)), ((), ())),
        preferred_element_type=jnp.float32,
    ).astype(jnp.bfloat16)
    head_cot, column_part = (
        lax.all_to_all(d_attn[None], "sp", split_axis=2, concat_axis=1, tiled=True),
        lax.all_to_all(d_out, "sp", split_axis=2, concat_axis=1, tiled=True),
    )
    grad_weight = lax.psum_scatter(
        lax.dot_general(
            whole_output,
            column_part[0],
            (((0,), (0,)), ((), ())),
            preferred_element_type=jnp.float32,
        ),
        "dp",
        scatter_dimension=0,
        tiled=True,
    )
    head_cols = query.shape[2]
    head_count = cum.shape[1]
    head_width = head_cols // head_count
    seq_length = query.shape[1]
    own_output = lax.dynamic_slice_in_dim(
        whole_output, lax.axis_index("sp") * head_cols, head_cols, 1
    )

    def heads_first(matrix):
        return jnp.transpose(matrix.reshape(seq_length, head_count, head_width), (1, 0, 2))

    def tokens_first(matrix):
        return jnp.transpose(matrix, (1, 0, 2)).reshape(1, seq_length, head_cols)

    grads = head_grads(
        heads_first(query[0]),
        heads_first(keys[0]),
        heads_first(values[0]),
        heads_first(own_output),
        heads_first(head_cot[0]),
        cum[0],
    )
    query_grad, key_grad, value_grad = (
        lax.all_to_all(tokens_first(grads[0]), "sp", split_axis=1, concat_axis=2, tiled=True),
        lax.all_to_all(tokens_first(grads[1]), "sp", split_axis=1, concat_axis=2, tiled=True),
        lax.all_to_all(tokens_first(grads[2]), "sp", split_axis=1, concat_axis=2, tiled=True),
    )
    return (query_grad, key_grad, value_grad, grads[3][None], grad_weight)


def fits(sizes, args):
    split, groups = sizes
    query, output, cum, d_out, w_out = args[0], args[3], args[4], args[5], args[6]
    _, attn = query.shape[1:]
    width, heads = attn // split, cum.shape[1] // split
    head_width = width // max(heads, 1)
    return (
        split == 4
        and groups == 2 * split
        and width == 2 * LANES
        and heads * head_width == width
        and LANES % head_width == 0
        and 8 % heads == 0
        and head_width**0.5 % 1 == 0
        and head_width & (head_width - 1) == 0
        and w_out.shape[0] // groups == LANES
        and output.shape[2] == attn
        and d_out.shape[1] // split == LANES
        and d_out.shape[2] % (split * LANES) == 0
    )


def solution(mesh):
    placed = (
        P("dp", None, "sp"),
        P("dp", None, "sp"),
        P("dp", None, "sp"),
        P("dp", None, None),
        P("dp", "sp", None),
        P("dp", "sp", None),
        P("dp", None),
    )
    sizes = (mesh.shape["sp"], mesh.shape["dp"])

    def step(*args):
        body = functools.partial(fused_shards, sizes) if fits(sizes, args) else shards
        return jax.shard_map(
            body,
            mesh=mesh,
            in_specs=placed,
            out_specs=(
                P("dp", "sp", None),
                P("dp", "sp", None),
                P("dp", "sp", None),
                P("dp", "sp", None),
                P("dp", "sp"),
            ),
            check_vma=False,
        )(*args)

    return step
```

```python
import functools

import jax
import jax.numpy as jnp
from jax import lax
from jax.experimental import pallas as pl
from jax.experimental.pallas import tpu as pltpu
from jax.sharding import PartitionSpec as P


LANES = 128
F32 = jnp.float32
BF16 = jnp.bfloat16
KERNEL_BYTES = 16 << 20


def dot_nn(left, right):
    return lax.dot_general(left, right, (((1,), (0,)), ((), ())), preferred_element_type=F32)


def dot_nt(left, right):
    return lax.dot_general(left, right, (((1,), (1,)), ((), ())), preferred_element_type=F32)


def window(index, size):
    return pl.ds(pl.multiple_of(index * size, size), size)


def lane_head(value, head, width):
    lane = lax.broadcasted_iota(jnp.int32, value.shape, 1)
    inside = (lane >= head * width) & (lane < (head + 1) * width)
    return jnp.where(inside, value, jnp.zeros_like(value))


def row_head(value, head, width):
    row = lax.broadcasted_iota(jnp.int32, value.shape, 0)
    inside = (row >= head * width) & (row < (head + 1) * width)
    return jnp.where(inside, value, jnp.zeros_like(value))


def prep_kernel(halves, d_out_hbm, w_out_hbm, *refs):
    parts, sems = refs[:-1], refs[-1]
    width = parts[0].shape[1]
    rows = parts[2].shape[0]
    chip = lax.axis_index("sp") // 2
    sources = [d_out_hbm.at[:, window(1 - chip, width)], d_out_hbm.at[:, window(chip, width)]]
    sources += [w_out_hbm.at[pl.ds(half * rows, rows), :] for half in range(halves)]
    copies = []
    for index, (source, part) in enumerate(zip(sources, parts)):
        copies.append(pltpu.make_async_copy(source, part, sems.at[index]))
        copies[-1].start()
    for copy in copies:
        copy.wait()


def prob_kernel(heads, query_hbm, keys_hbm, output_hbm, cum_hbm, *refs):
    prob_ref, out_t_ref, keys_t_ref, query_ref, keys_ref, output_ref, cum_ref, sems = refs
    copies = []
    for index, (source, part) in enumerate(
        (
            (cum_hbm, cum_ref),
            (query_hbm, query_ref),
            (keys_hbm, keys_ref),
            (output_hbm, output_ref),
        )
    ):
        copies.append(pltpu.make_async_copy(source, part, sems.at[index]))
        copies[-1].start()
    for copy in copies[:3]:
        copy.wait()
    length, width = query_ref.shape
    head_width = width // heads
    per_group = LANES // head_width
    scale = jnp.asarray(head_width**-0.5, BF16)
    cum = cum_ref[...]
    cum_cols = jnp.transpose(jnp.concatenate([cum] + [jnp.zeros_like(cum)] * (8 // heads - 1), 0))
    key_at = lax.broadcasted_iota(jnp.int32, (LANES, LANES), 0)
    query_at = lax.broadcasted_iota(jnp.int32, (LANES, LANES), 1)
    causal = key_at <= query_at
    for head in range(heads):
        lanes = pl.ds(head // per_group * LANES, LANES)
        keys_head = lane_head(keys_ref[:, lanes], head % per_group, head_width)
        cum_key = cum_cols[:, head : head + 1]
        for block in range(length // LANES):
            rows = (block + 1) * LANES
            own = pl.ds(block * LANES, LANES)
            scores = dot_nt(keys_head[:rows], query_ref[own, lanes] * scale)
            cum_query = cum[head : head + 1, block * LANES : rows]
            scores = scores - cum_key[:rows]
            last = jnp.where(causal, scores[block * LANES :], -1e30)
            scores = jnp.concatenate([scores[: block * LANES], last], 0) if block else last
            top = jnp.max(scores, axis=0, keepdims=True) + cum_query
            weights = jnp.exp(scores + (cum_query - top))
            weights = weights * (1.0 / jnp.sum(weights, axis=0, keepdims=True))
            prob_ref[head, :rows, own] = weights.astype(BF16)
    keys_t_ref[...] = jnp.transpose(keys_ref[...] * scale)
    copies[3].wait()
    out_t_ref[...] = jnp.transpose(output_ref[...])


def weight_kernel(inner, out_t_ref, own_ref, near_ref, far_ref, cross_ref, *refs):
    keep_ref, give_ref, stay_ref, send_ref, columns_ref = refs
    me, place = lax.axis_index("sp"), lax.axis_index("dp")
    outer, mine = place // inner, place % inner
    tokens = own_ref.shape[0]
    half = keep_ref.shape[2]
    block_rows = keep_ref.shape[1]
    for step, (shard, at) in enumerate(
        ((own_ref, me % 2), (near_ref, me), (far_ref, me % 2), (cross_ref, me % 2))
    ):
        columns_ref[window(me ^ step, tokens), :] = shard[:, window(at, 2 * half)]
    columns = columns_ref[...]
    for step in range(keep_ref.shape[0]):
        to_ref = (stay_ref, send_ref)[step % 2]
        for index, by_inner in enumerate((keep_ref, give_ref)):
            block = (outer ^ step) * inner + (mine ^ index)
            part = dot_nn(out_t_ref[window(block, block_rows), :], columns)
            by_inner[step] = part[:, :half].astype(by_inner.dtype)
            to_ref[step // 2, index] = part[:, half:].astype(to_ref.dtype)


def pair_merge_kernel(stay_ref, got_ref, own_ref, send_ref):
    total = stay_ref[...] + got_ref[...].astype(F32)
    own_ref[...] = total[0]
    send_ref[...] = total[1].astype(BF16)


def inner_merge_kernel(keep_ref, got_ref, own_ref, *send_refs):
    total = keep_ref[...] + got_ref[...].astype(F32)
    own_ref[...] = total[0]
    for step, send_ref in enumerate(send_refs, 1):
        send_ref[...] = total[step].astype(BF16)


def finish_kernel(first_ref, second_ref, last_ref, *refs):
    got_refs, total_ref = refs[:-1], refs[-1]
    first = first_ref[...]
    half = first.shape[1]
    for got_ref in got_refs:
        first = first + got_ref[...].astype(F32)
    total_ref[:, :half] = first
    total_ref[:, half:] = second_ref[...] + last_ref[...].astype(F32)


def grads_kernel(other, heads, steps, pieces, *refs):
    (prob_ref, query_ref, keys_t_ref, values_ref, out_t_ref), refs = refs[:5], refs[5:]
    near_ref, refs = refs[0], refs[1:]
    parted, refs = ((0, refs[:2]), (2, refs[2:4]), (3, refs[4:6])), refs[6:]
    weights, refs = refs[:pieces], refs[pieces:]
    before = ()
    if other:
        before, refs = refs[:steps], refs[steps:]
    slot_refs, refs = refs[:steps], refs[steps:]
    cum_ref, cot_ref, score_ref, query_grad_ref, key_grad_ref, value_grad_ref, sums_ref = refs[:7]
    weight_ref = refs[7]
    me = lax.axis_index("sp")
    group = lax.axis_index("dp") % 2
    if other:
        group = 1 - group
    length, width = query_ref.shape
    head_width = width // heads
    per_group = LANES // head_width
    tokens = near_ref.shape[0]
    scale = jnp.asarray(head_width**-0.5, BF16)
    piece_rows = LANES // pieces
    for index, piece in enumerate(weights):
        weight_ref[pl.ds(index * piece_rows, piece_rows), :] = piece[...]
    cot_ref[:, window(me ^ 1, tokens)] = dot_nt(weight_ref[...], near_ref[...]).astype(BF16)
    for step, (here, there) in parted:
        half = here.shape[1]
        cot = dot_nt(weight_ref[:, window(me // 2, half)], here[...])
        cot = cot + dot_nt(weight_ref[:, window(1 - me // 2, half)], there[...])
        cot_ref[:, window(me ^ step, tokens)] = cot.astype(BF16)
    lanes = window(group, LANES)
    cot = cot_ref[...]
    query = query_ref[:, lanes] * scale
    keys_t = keys_t_ref[lanes, :]
    out_t = out_t_ref[window(me * (width // LANES) + group, LANES), :]
    product = cot.astype(F32) * out_t.astype(F32)
    blocks = length // LANES
    key_grads, value_grads = [0.0] * blocks, [0.0] * blocks
    query_grads = [0.0] * blocks
    sum_columns, sum_rows = [], []
    cot_heads = [row_head(cot, head, head_width) for head in range(per_group)]
    query_heads = [lane_head(query, head, head_width) for head in range(per_group)]
    keys_heads = [row_head(keys_t, head, head_width) for head in range(per_group)]
    dots_heads = []
    for head in range(per_group):
        dots = product[head * head_width : (head + 1) * head_width]
        dots_heads.append(jnp.sum(dots, axis=0, keepdims=True))
    rows_sums = [[0.0] * blocks for _ in range(per_group)]
    for block in range(blocks):
        own = pl.ds(block * LANES, LANES)
        at = slice(block * LANES, (block + 1) * LANES)
        for head in range(per_group):
            index = group * per_group + head
            rows = (block + 1) * LANES
            d_prob = dot_nn(values_ref[:rows, lanes], cot_heads[head][:, at])
            d_score = prob_ref[index, :rows, own].astype(F32) * (d_prob - dots_heads[head][:, at])
            rows_sums[head][block] = jnp.sum(d_score, axis=0, keepdims=True)
            if block:
                sums_ref[head, : block * LANES, :] += d_score[: block * LANES]
            sums_ref[head, own, :] = d_score[block * LANES :]
            score_ref[head, :rows, own] = d_score.astype(BF16)
    for block in range(blocks):
        own = pl.ds(block * LANES, LANES)
        start, rows = block * LANES, (block + 1) * LANES
        for head in range(per_group):
            index = group * per_group + head
            query_grads[block] += dot_nn(keys_heads[head][:, :rows], score_ref[head, :rows, own])
            key_grads[block] += dot_nn(score_ref[head, own, start:], query_heads[head][start:])
            value_grads[block] += dot_nt(prob_ref[index, own, start:], cot_heads[head][:, start:])
    for head in range(per_group):
        sum_columns.append(jnp.sum(sums_ref[head], axis=1, keepdims=True))
        sum_rows.append(jnp.concatenate(rows_sums[head], 1))
    lane = lax.broadcasted_iota(jnp.int32, (length, LANES), 1)
    spread = jnp.zeros((length, LANES), F32)
    for head in range(per_group):
        spread = jnp.where(lane == head, sum_columns[head], spread)
    cum_ref[...] = jnp.concatenate(sum_rows, 0) - jnp.transpose(spread)[:per_group]
    for block in range(blocks):
        own = pl.ds(block * LANES, LANES)
        query_grad_ref[own, :] = jnp.transpose(query_grads[block]).astype(BF16)
        key_grad_ref[own, :] = key_grads[block].astype(BF16)
        value_grad_ref[own, :] = value_grads[block].astype(BF16)
    kinds = 3
    for step, slot_ref in enumerate(slot_refs):
        here = window(me ^ step, tokens)
        if other:
            slot_ref[:kinds] = before[step][...]
        start = kinds if other else 0
        slot_ref[start] = query_grad_ref[here, :]
        slot_ref[start + 1] = key_grad_ref[here, :]
        slot_ref[start + 2] = value_grad_ref[here, :]


def place_kernel(*refs):
    parts, (first_cum_ref, second_cum_ref) = refs[:-6], refs[-6:-4]
    grad_refs, cum_ref = refs[-4:-1], refs[-1]
    me, mine = lax.axis_index("sp"), lax.axis_index("dp") % 2
    for step, part in enumerate(parts):
        for index, group in enumerate((mine, 1 - mine)):
            columns = window((me ^ step) * 2 + group, LANES)
            for kind, grad_ref in enumerate(grad_refs):
                grad_ref[:, columns] = part[index * len(grad_refs) + kind]
    low, high = first_cum_ref[...], second_cum_ref[...]
    swap = jnp.full(low.shape, mine, jnp.int32) == 1
    cum_ref[...] = jnp.concatenate(
        [jnp.where(swap, high, low), jnp.where(swap, low, high)], 0
    )


def call(kernel, outs, args, scratch=(), inputs=pltpu.VMEM, copies=0):
    scratch_shapes = [pltpu.VMEM(shape, kind) for shape, kind in scratch]
    if copies:
        scratch_shapes.append(pltpu.SemaphoreType.DMA((copies,)))
    run = pl.pallas_call(
        kernel,
        out_shape=[jax.ShapeDtypeStruct(shape, kind) for shape, kind in outs],
        in_specs=[pl.BlockSpec(memory_space=inputs)] * len(args),
        out_specs=[pl.BlockSpec(memory_space=pltpu.VMEM)] * len(outs),
        scratch_shapes=scratch_shapes,
        compiler_params=pltpu.CompilerParams(vmem_limit_bytes=KERNEL_BYTES),
    )
    if inputs is pltpu.HBM:
        args = [pltpu.with_memory_space_constraint(array, inputs) for array in args]
    return run(*args)


def fused_shards(sizes, query, keys, values, output, cum, d_out, w_out):
    split, groups = sizes
    inner = groups // split
    query, keys, values, output, cum, d_out = (
        query[0], keys[0], values[0], output[0], cum[0], d_out[0]
    )
    length, width = query.shape
    heads = cum.shape[0]
    head_width = width // heads
    per_group = LANES // head_width
    tokens, model = d_out.shape
    block_rows = w_out.shape[0]
    attn = output.shape[1]

    def device(shard, group):
        return shard * groups + group

    def sp_swap(array, step):
        return lax.ppermute(array, "sp", [(i, i ^ step) for i in range(split)])

    def inner_swap(array):
        return lax.ppermute(array, "dp", [(i, i ^ 1) for i in range(groups)])

    def outer_swap(array, step):
        pairs = []
        for outer in range(split):
            for at in range(inner):
                pairs.append((outer * inner + at, (outer ^ step) * inner + at))
        return lax.ppermute(array, "dp", pairs)

    def spread(replica, half):
        return (replica + half) % split

    halves = split
    half_rows = block_rows // halves
    away, home, *cuts = call(
        functools.partial(prep_kernel, halves),
        [((tokens, model // 2), BF16)] * 2 + [((half_rows, model), BF16)] * halves,
        (d_out, w_out),
        inputs=pltpu.HBM,
        copies=2 + halves,
    )
    first_rows = []
    for half in range(halves):
        pairs = []
        for shard in range(split):
            for at in range(inner):
                for replica in range(split):
                    source = device(replica, shard * inner + at)
                    pairs.append((source, device(shard, spread(replica, half) * inner + at)))
        first_rows.append(lax.ppermute(cuts[half], ("sp", "dp"), pairs))
    second_rows = [inner_swap(piece) for piece in first_rows]

    near = sp_swap(d_out, 1)
    far_here = sp_swap(away, 2)
    far_there = sp_swap(home, 2)
    cross_here = sp_swap(far_here, 1)
    cross_there = sp_swap(far_there, 1)

    prob, out_t, keys_t = call(
        functools.partial(prob_kernel, heads),
        [((heads, length, length), BF16), ((attn, length), BF16), ((width, length), BF16)],
        (query, keys, output, cum),
        [((length, width), BF16)] * 2 + [((length, attn), BF16), ((heads, length), F32)],
        inputs=pltpu.HBM,
        copies=4,
    )
    half = model // split // 2
    share = (block_rows, half)
    keep, give, stay, pair = call(
        functools.partial(weight_kernel, inner),
        [
            ((split, *share), F32),
            ((split, *share), BF16),
            ((split // 2, inner, *share), F32),
            ((split // 2, inner, *share), BF16),
        ],
        (out_t, home, near, far_here, cross_here),
        [((length, 2 * half), BF16)],
    )
    stay, pair = call(
        pair_merge_kernel,
        [((inner, *share), F32), ((inner, *share), BF16)],
        (stay, outer_swap(pair, 1)),
    )
    second, last = call(
        pair_merge_kernel, [(share, F32), (share, BF16)], (stay, outer_swap(pair, 2))
    )
    last = inner_swap(last)
    first, *parts = call(
        inner_merge_kernel, [(share, F32)] + [(share, BF16)] * (split - 1), (keep, inner_swap(give))
    )
    parts = [outer_swap(part, step) for step, part in enumerate(parts, 1)]
    grad_weight, = call(
        finish_kernel, [((block_rows, 2 * half), F32)], (first, second, last, *parts)
    )

    slots, cums = [], []
    for other, rows in ((False, first_rows), (True, second_rows)):
        kinds = 6 if other else 3
        *slots, part_cum = call(
            functools.partial(grads_kernel, other, heads, split, halves),
            [((kinds, tokens, LANES), BF16)] * split + [((per_group, length), F32)],
            (
                prob, query, keys_t, values, out_t, near,
                home, away, far_here, far_there, cross_here, cross_there, *rows, *slots,
            ),
            [
                ((LANES, length), BF16),
                ((per_group, length, length), BF16),
                ((length, LANES), BF16),
                ((length, LANES), BF16),
                ((length, LANES), BF16),
                ((per_group, length, LANES), F32),
                ((LANES, model), BF16),
            ],
        )
        cums.append(part_cum)
    arrived = [slots[0]] + [sp_swap(slots[i], i) for i in range(1, split)]
    query_grad, key_grad, value_grad, cum_grad = call(
        place_kernel, [((tokens, attn), BF16)] * 3 + [((heads, length), F32)], (*arrived, *cums)
    )
    return query_grad[None], key_grad[None], value_grad[None], cum_grad[None], grad_weight


def head_grads(query, keys, values, output, cotangent, cum):
    _, length, head_width = query.shape
    span_rows = min(512, length)
    score_scale = head_width ** (-0.5)
    row_dots = jnp.sum(cotangent.astype(jnp.float32) * output.astype(jnp.float32), axis=2)
    positions = jnp.arange(length)

    def product(left, right, form):
        return jnp.einsum(form, left, right, preferred_element_type=jnp.float32)

    def advance(totals, block_index):
        key_grad, value_grad, cum_grad = totals
        offset = block_index * span_rows
        query_blk = lax.dynamic_slice_in_dim(query, offset, span_rows, 1)
        cot_blk = lax.dynamic_slice_in_dim(cotangent, offset, span_rows, 1)
        cum_blk = lax.dynamic_slice_in_dim(cum, offset, span_rows, 1)
        dots_blk = lax.dynamic_slice_in_dim(row_dots, offset, span_rows, 1)
        scores = product(query_blk, keys, "hqe,hke->hqk") * score_scale
        scores = scores + cum_blk[:, :, None] - cum[:, None, :]
        query_pos = offset + jnp.arange(span_rows)
        causal = positions[None, :] <= query_pos[:, None]
        scores = jnp.where(causal[None], scores, -1e30)
        row_max = jnp.max(scores, axis=2, keepdims=True)
        weights = jnp.exp(scores - row_max)
        weights = weights / jnp.sum(weights, axis=2, keepdims=True)
        weights_b = weights.astype(jnp.bfloat16)
        d_prob = product(cot_blk, values, "hqe,hke->hqk")
        d_score = weights * (d_prob - dots_blk[:, :, None])
        score_b = d_score.astype(jnp.bfloat16)
        query_grad = (product(score_b, keys, "hqk,hke->hqe") * score_scale).astype(jnp.bfloat16)
        key_grad = key_grad + product(score_b, query_blk, "hqk,hqe->hke") * score_scale
        value_grad = value_grad + product(weights_b, cot_blk, "hqk,hqe->hke")
        cum_grad = cum_grad - jnp.sum(d_score, axis=1)
        own_part = lax.dynamic_slice_in_dim(cum_grad, offset, span_rows, 1) + jnp.sum(
            d_score, axis=2
        )
        cum_grad = lax.dynamic_update_slice_in_dim(cum_grad, own_part, offset, 1)
        return ((key_grad, value_grad, cum_grad), query_grad)

    start_state = (
        jnp.zeros(query.shape, jnp.float32),
        jnp.zeros(query.shape, jnp.float32),
        jnp.zeros(cum.shape, jnp.float32),
    )
    totals, query_blocks = lax.scan(advance, start_state, jnp.arange(length // span_rows))
    query_grad = jnp.transpose(query_blocks, (1, 0, 2, 3)).reshape(query.shape)
    return (query_grad, totals[0].astype(jnp.bfloat16), totals[1].astype(jnp.bfloat16), totals[2])


def shards(query, keys, values, output, cum, d_out, w_out):
    local_rows = d_out[0]
    whole_output = output[0]
    d_attn = lax.dot_general(
        local_rows,
        lax.all_gather(w_out, "dp", axis=0, tiled=True),
        (((1,), (1,)), ((), ())),
        preferred_element_type=jnp.float32,
    ).astype(jnp.bfloat16)
    head_cot, column_part = (
        lax.all_to_all(d_attn[None], "sp", split_axis=2, concat_axis=1, tiled=True),
        lax.all_to_all(d_out, "sp", split_axis=2, concat_axis=1, tiled=True),
    )
    grad_weight = lax.psum_scatter(
        lax.dot_general(
            whole_output,
            column_part[0],
            (((0,), (0,)), ((), ())),
            preferred_element_type=jnp.float32,
        ),
        "dp",
        scatter_dimension=0,
        tiled=True,
    )
    head_cols = query.shape[2]
    head_count = cum.shape[1]
    head_width = head_cols // head_count
    seq_length = query.shape[1]
    own_output = lax.dynamic_slice_in_dim(
        whole_output, lax.axis_index("sp") * head_cols, head_cols, 1
    )

    def heads_first(matrix):
        return jnp.transpose(matrix.reshape(seq_length, head_count, head_width), (1, 0, 2))

    def tokens_first(matrix):
        return jnp.transpose(matrix, (1, 0, 2)).reshape(1, seq_length, head_cols)

    grads = head_grads(
        heads_first(query[0]),
        heads_first(keys[0]),
        heads_first(values[0]),
        heads_first(own_output),
        heads_first(head_cot[0]),
        cum[0],
    )
    query_grad, key_grad, value_grad = (
        lax.all_to_all(tokens_first(grads[0]), "sp", split_axis=1, concat_axis=2, tiled=True),
        lax.all_to_all(tokens_first(grads[1]), "sp", split_axis=1, concat_axis=2, tiled=True),
        lax.all_to_all(tokens_first(grads[2]), "sp", split_axis=1, concat_axis=2, tiled=True),
    )
    return (query_grad, key_grad, value_grad, grads[3][None], grad_weight)


def fits(sizes, args):
    split, groups = sizes
    query, output, cum, d_out, w_out = args[0], args[3], args[4], args[5], args[6]
    _, attn = query.shape[1:]
    width, heads = attn // split, cum.shape[1] // split
    head_width = width // max(heads, 1)
    return (
        split == 4
        and groups == 2 * split
        and width == 2 * LANES
        and heads * head_width == width
        and LANES % head_width == 0
        and 8 % heads == 0
        and head_width**0.5 % 1 == 0
        and head_width & (head_width - 1) == 0
        and w_out.shape[0] // groups == LANES
        and output.shape[2] == attn
        and d_out.shape[1] // split == LANES
        and d_out.shape[2] % (split * LANES) == 0
    )


def solution(mesh):
    placed = (
        P("dp", None, "sp"),
        P("dp", None, "sp"),
        P("dp", None, "sp"),
        P("dp", None, None),
        P("dp", "sp", None),
        P("dp", "sp", None),
        P("dp", None),
    )
    sizes = (mesh.shape["sp"], mesh.shape["dp"])

    def step(*args):
        body = functools.partial(fused_shards, sizes) if fits(sizes, args) else shards
        return jax.shard_map(
            body,
            mesh=mesh,
            in_specs=placed,
            out_specs=(
                P("dp", "sp", None),
                P("dp", "sp", None),
                P("dp", "sp", None),
                P("dp", "sp", None),
                P("dp", "sp"),
            ),
            check_vma=False,
        )(*args)

    return step
```

```python
import functools

import jax
import jax.numpy as jnp
from jax import lax
from jax.experimental import pallas as pl
from jax.experimental.pallas import tpu as pltpu
from jax.sharding import PartitionSpec as P


LANES = 128
F32 = jnp.float32
BF16 = jnp.bfloat16
KERNEL_BYTES = 16 << 20


def dot_nn(left, right):
    return lax.dot_general(left, right, (((1,), (0,)), ((), ())), preferred_element_type=F32)


def dot_nt(left, right):
    return lax.dot_general(left, right, (((1,), (1,)), ((), ())), preferred_element_type=F32)


def window(index, size):
    return pl.ds(pl.multiple_of(index * size, size), size)


def lane_head(value, head, width):
    lane = lax.broadcasted_iota(jnp.int32, value.shape, 1)
    inside = (lane >= head * width) & (lane < (head + 1) * width)
    return jnp.where(inside, value, jnp.zeros_like(value))


def row_head(value, head, width):
    row = lax.broadcasted_iota(jnp.int32, value.shape, 0)
    inside = (row >= head * width) & (row < (head + 1) * width)
    return jnp.where(inside, value, jnp.zeros_like(value))


def prep_kernel(halves, d_out_hbm, w_out_hbm, *refs):
    parts, sems = refs[:-1], refs[-1]
    width = parts[0].shape[1]
    rows = parts[2].shape[0]
    chip = lax.axis_index("sp") // 2
    sources = [d_out_hbm.at[:, window(1 - chip, width)], d_out_hbm.at[:, window(chip, width)]]
    sources += [w_out_hbm.at[pl.ds(half * rows, rows), :] for half in range(halves)]
    copies = []
    for index, (source, part) in enumerate(zip(sources, parts)):
        copies.append(pltpu.make_async_copy(source, part, sems.at[index]))
        copies[-1].start()
    for copy in copies:
        copy.wait()


def prob_kernel(heads, query_hbm, keys_hbm, output_hbm, cum_hbm, *refs):
    prob_ref, out_t_ref, keys_t_ref, query_ref, keys_ref, output_ref, cum_ref, sems = refs
    copies = []
    for index, (source, part) in enumerate(
        (
            (cum_hbm, cum_ref),
            (query_hbm, query_ref),
            (keys_hbm, keys_ref),
            (output_hbm, output_ref),
        )
    ):
        copies.append(pltpu.make_async_copy(source, part, sems.at[index]))
        copies[-1].start()
    for copy in copies[:3]:
        copy.wait()
    length, width = query_ref.shape
    head_width = width // heads
    per_group = LANES // head_width
    scale = jnp.asarray(head_width**-0.5, BF16)
    cum = cum_ref[...]
    cum_cols = jnp.transpose(jnp.concatenate([cum] + [jnp.zeros_like(cum)] * (8 // heads - 1), 0))
    key_at = lax.broadcasted_iota(jnp.int32, (LANES, LANES), 0)
    query_at = lax.broadcasted_iota(jnp.int32, (LANES, LANES), 1)
    causal = key_at <= query_at
    for head in range(heads):
        lanes = pl.ds(head // per_group * LANES, LANES)
        keys_head = lane_head(keys_ref[:, lanes], head % per_group, head_width)
        cum_key = cum_cols[:, head : head + 1]
        for block in range(length // LANES):
            rows = (block + 1) * LANES
            own = pl.ds(block * LANES, LANES)
            scores = dot_nt(keys_head[:rows], query_ref[own, lanes] * scale)
            cum_query = cum[head : head + 1, block * LANES : rows]
            scores = scores - cum_key[:rows]
            last = jnp.where(causal, scores[block * LANES :], -1e30)
            scores = jnp.concatenate([scores[: block * LANES], last], 0) if block else last
            top = jnp.max(scores, axis=0, keepdims=True) + cum_query
            weights = jnp.exp(scores + (cum_query - top))
            weights = weights * (1.0 / jnp.sum(weights, axis=0, keepdims=True))
            prob_ref[head, :rows, own] = weights.astype(BF16)
    keys_t_ref[...] = jnp.transpose(keys_ref[...] * scale)
    copies[3].wait()
    out_t_ref[...] = jnp.transpose(output_ref[...])


def weight_kernel(inner, out_t_ref, own_ref, near_ref, far_ref, cross_ref, *refs):
    keep_ref, give_ref, stay_ref, send_ref, columns_ref = refs
    me, place = lax.axis_index("sp"), lax.axis_index("dp")
    outer, mine = place // inner, place % inner
    tokens = own_ref.shape[0]
    half = keep_ref.shape[2]
    block_rows = keep_ref.shape[1]
    for step, (shard, at) in enumerate(
        ((own_ref, me % 2), (near_ref, me), (far_ref, me % 2), (cross_ref, me % 2))
    ):
        columns_ref[window(me ^ step, tokens), :] = shard[:, window(at, 2 * half)]
    columns = columns_ref[...]
    for step in range(keep_ref.shape[0]):
        to_ref = (stay_ref, send_ref)[step % 2]
        for index, by_inner in enumerate((keep_ref, give_ref)):
            block = (outer ^ step) * inner + (mine ^ index)
            part = dot_nn(out_t_ref[window(block, block_rows), :], columns)
            by_inner[step] = part[:, :half].astype(by_inner.dtype)
            to_ref[step // 2, index] = part[:, half:].astype(to_ref.dtype)


def pair_merge_kernel(stay_ref, got_ref, own_ref, send_ref):
    total = stay_ref[...] + got_ref[...].astype(F32)
    own_ref[...] = total[0]
    send_ref[...] = total[1].astype(BF16)


def inner_merge_kernel(keep_ref, got_ref, own_ref, *send_refs):
    total = keep_ref[...] + got_ref[...].astype(F32)
    own_ref[...] = total[0]
    for step, send_ref in enumerate(send_refs, 1):
        send_ref[...] = total[step].astype(BF16)


def grads_kernel(other, heads, steps, pieces, *refs):
    (prob_ref, query_ref, keys_t_ref, values_ref, out_t_ref), refs = refs[:5], refs[5:]
    near_ref, refs = refs[0], refs[1:]
    parted, refs = ((0, refs[:2]), (2, refs[2:4]), (3, refs[4:6])), refs[6:]
    weights, refs = refs[:pieces], refs[pieces:]
    before = ()
    if other:
        before, refs = refs[:steps], refs[steps:]
    slot_refs, refs = refs[:steps], refs[steps:]
    cum_ref, cot_ref, score_ref, query_grad_ref, key_grad_ref, value_grad_ref, sums_ref = refs[:7]
    weight_ref = refs[7]
    me = lax.axis_index("sp")
    group = lax.axis_index("dp") % 2
    if other:
        group = 1 - group
    length, width = query_ref.shape
    head_width = width // heads
    per_group = LANES // head_width
    tokens = near_ref.shape[0]
    scale = jnp.asarray(head_width**-0.5, BF16)
    piece_rows = LANES // pieces
    for index, piece in enumerate(weights):
        weight_ref[pl.ds(index * piece_rows, piece_rows), :] = piece[...]
    cot_ref[:, window(me ^ 1, tokens)] = dot_nt(weight_ref[...], near_ref[...]).astype(BF16)
    for step, (here, there) in parted:
        half = here.shape[1]
        cot = dot_nt(weight_ref[:, window(me // 2, half)], here[...])
        cot = cot + dot_nt(weight_ref[:, window(1 - me // 2, half)], there[...])
        cot_ref[:, window(me ^ step, tokens)] = cot.astype(BF16)
    lanes = window(group, LANES)
    cot = cot_ref[...]
    query = query_ref[:, lanes] * scale
    keys_t = keys_t_ref[lanes, :]
    out_t = out_t_ref[window(me * (width // LANES) + group, LANES), :]
    product = cot.astype(F32) * out_t.astype(F32)
    blocks = length // LANES
    key_grads, value_grads = [0.0] * blocks, [0.0] * blocks
    query_grads = [0.0] * blocks
    sum_columns, sum_rows = [], []
    cot_heads = [row_head(cot, head, head_width) for head in range(per_group)]
    query_heads = [lane_head(query, head, head_width) for head in range(per_group)]
    keys_heads = [row_head(keys_t, head, head_width) for head in range(per_group)]
    dots_heads = []
    for head in range(per_group):
        dots = product[head * head_width : (head + 1) * head_width]
        dots_heads.append(jnp.sum(dots, axis=0, keepdims=True))
    rows_sums = [[0.0] * blocks for _ in range(per_group)]
    for block in range(blocks):
        own = pl.ds(block * LANES, LANES)
        at = slice(block * LANES, (block + 1) * LANES)
        for head in range(per_group):
            index = group * per_group + head
            rows = (block + 1) * LANES
            d_prob = dot_nn(values_ref[:rows, lanes], cot_heads[head][:, at])
            d_score = prob_ref[index, :rows, own].astype(F32) * (d_prob - dots_heads[head][:, at])
            rows_sums[head][block] = jnp.sum(d_score, axis=0, keepdims=True)
            if block:
                sums_ref[head, : block * LANES, :] += d_score[: block * LANES]
            sums_ref[head, own, :] = d_score[block * LANES :]
            score_ref[head, :rows, own] = d_score.astype(BF16)
    for block in range(blocks):
        own = pl.ds(block * LANES, LANES)
        start, rows = block * LANES, (block + 1) * LANES
        for head in range(per_group):
            index = group * per_group + head
            query_grads[block] += dot_nn(keys_heads[head][:, :rows], score_ref[head, :rows, own])
            key_grads[block] += dot_nn(score_ref[head, own, start:], query_heads[head][start:])
            value_grads[block] += dot_nt(prob_ref[index, own, start:], cot_heads[head][:, start:])
    for head in range(per_group):
        sum_columns.append(jnp.sum(sums_ref[head], axis=1, keepdims=True))
        sum_rows.append(jnp.concatenate(rows_sums[head], 1))
    lane = lax.broadcasted_iota(jnp.int32, (length, LANES), 1)
    spread = jnp.zeros((length, LANES), F32)
    for head in range(per_group):
        spread = jnp.where(lane == head, sum_columns[head], spread)
    cum_ref[...] = jnp.concatenate(sum_rows, 0) - jnp.transpose(spread)[:per_group]
    for block in range(blocks):
        own = pl.ds(block * LANES, LANES)
        query_grad_ref[own, :] = jnp.transpose(query_grads[block]).astype(BF16)
        key_grad_ref[own, :] = key_grads[block].astype(BF16)
        value_grad_ref[own, :] = value_grads[block].astype(BF16)
    kinds = 3
    for step, slot_ref in enumerate(slot_refs):
        here = window(me ^ step, tokens)
        if other:
            slot_ref[:kinds] = before[step][...]
        start = kinds if other else 0
        slot_ref[start] = query_grad_ref[here, :]
        slot_ref[start + 1] = key_grad_ref[here, :]
        slot_ref[start + 2] = value_grad_ref[here, :]


def place_kernel(steps, *refs):
    parts, (first_cum_ref, second_cum_ref) = refs[:steps], refs[steps : steps + 2]
    (first_ref, second_ref, last_ref), got_refs = refs[steps + 2 : steps + 5], refs[steps + 5 : -5]
    grad_refs, cum_ref, total_ref = refs[-5:-2], refs[-2], refs[-1]
    me, mine = lax.axis_index("sp"), lax.axis_index("dp") % 2
    for step, part in enumerate(parts):
        for index, group in enumerate((mine, 1 - mine)):
            columns = window((me ^ step) * 2 + group, LANES)
            for kind, grad_ref in enumerate(grad_refs):
                grad_ref[:, columns] = part[index * len(grad_refs) + kind]
    low, high = first_cum_ref[...], second_cum_ref[...]
    swap = jnp.full(low.shape, mine, jnp.int32) == 1
    cum_ref[...] = jnp.concatenate(
        [jnp.where(swap, high, low), jnp.where(swap, low, high)], 0
    )
    first = first_ref[...]
    half = first.shape[1]
    for got_ref in got_refs:
        first = first + got_ref[...].astype(F32)
    total_ref[:, :half] = first
    total_ref[:, half:] = second_ref[...] + last_ref[...].astype(F32)


def call(kernel, outs, args, scratch=(), inputs=pltpu.VMEM, copies=0):
    scratch_shapes = [pltpu.VMEM(shape, kind) for shape, kind in scratch]
    if copies:
        scratch_shapes.append(pltpu.SemaphoreType.DMA((copies,)))
    run = pl.pallas_call(
        kernel,
        out_shape=[jax.ShapeDtypeStruct(shape, kind) for shape, kind in outs],
        in_specs=[pl.BlockSpec(memory_space=inputs)] * len(args),
        out_specs=[pl.BlockSpec(memory_space=pltpu.VMEM)] * len(outs),
        scratch_shapes=scratch_shapes,
        compiler_params=pltpu.CompilerParams(vmem_limit_bytes=KERNEL_BYTES),
    )
    if inputs is pltpu.HBM:
        args = [pltpu.with_memory_space_constraint(array, inputs) for array in args]
    return run(*args)


def fused_shards(sizes, query, keys, values, output, cum, d_out, w_out):
    split, groups = sizes
    inner = groups // split
    query, keys, values, output, cum, d_out = (
        query[0], keys[0], values[0], output[0], cum[0], d_out[0]
    )
    length, width = query.shape
    heads = cum.shape[0]
    head_width = width // heads
    per_group = LANES // head_width
    tokens, model = d_out.shape
    block_rows = w_out.shape[0]
    attn = output.shape[1]

    def device(shard, group):
        return shard * groups + group

    def sp_swap(array, step):
        return lax.ppermute(array, "sp", [(i, i ^ step) for i in range(split)])

    def inner_swap(array):
        return lax.ppermute(array, "dp", [(i, i ^ 1) for i in range(groups)])

    def outer_swap(array, step):
        pairs = []
        for outer in range(split):
            for at in range(inner):
                pairs.append((outer * inner + at, (outer ^ step) * inner + at))
        return lax.ppermute(array, "dp", pairs)

    def spread(replica, half):
        return (replica + half) % split

    halves = split
    half_rows = block_rows // halves
    away, home, *cuts = call(
        functools.partial(prep_kernel, halves),
        [((tokens, model // 2), BF16)] * 2 + [((half_rows, model), BF16)] * halves,
        (d_out, w_out),
        inputs=pltpu.HBM,
        copies=2 + halves,
    )
    first_rows = []
    for half in range(halves):
        pairs = []
        for shard in range(split):
            for at in range(inner):
                for replica in range(split):
                    source = device(replica, shard * inner + at)
                    pairs.append((source, device(shard, spread(replica, half) * inner + at)))
        first_rows.append(lax.ppermute(cuts[half], ("sp", "dp"), pairs))
    second_rows = [inner_swap(piece) for piece in first_rows]

    near = sp_swap(d_out, 1)
    far_here = sp_swap(away, 2)
    far_there = sp_swap(home, 2)
    cross_here = sp_swap(far_here, 1)
    cross_there = sp_swap(far_there, 1)

    prob, out_t, keys_t = call(
        functools.partial(prob_kernel, heads),
        [((heads, length, length), BF16), ((attn, length), BF16), ((width, length), BF16)],
        (query, keys, output, cum),
        [((length, width), BF16)] * 2 + [((length, attn), BF16), ((heads, length), F32)],
        inputs=pltpu.HBM,
        copies=4,
    )
    half = model // split // 2
    share = (block_rows, half)
    keep, give, stay, pair = call(
        functools.partial(weight_kernel, inner),
        [
            ((split, *share), F32),
            ((split, *share), BF16),
            ((split // 2, inner, *share), F32),
            ((split // 2, inner, *share), BF16),
        ],
        (out_t, home, near, far_here, cross_here),
        [((length, 2 * half), BF16)],
    )
    stay, pair = call(
        pair_merge_kernel,
        [((inner, *share), F32), ((inner, *share), BF16)],
        (stay, outer_swap(pair, 1)),
    )
    second, last = call(
        pair_merge_kernel, [(share, F32), (share, BF16)], (stay, outer_swap(pair, 2))
    )
    last = inner_swap(last)
    first, *parts = call(
        inner_merge_kernel, [(share, F32)] + [(share, BF16)] * (split - 1), (keep, inner_swap(give))
    )
    parts = [outer_swap(part, step) for step, part in enumerate(parts, 1)]
    slots, cums = [], []
    for other, rows in ((False, first_rows), (True, second_rows)):
        kinds = 6 if other else 3
        *slots, part_cum = call(
            functools.partial(grads_kernel, other, heads, split, halves),
            [((kinds, tokens, LANES), BF16)] * split + [((per_group, length), F32)],
            (
                prob, query, keys_t, values, out_t, near,
                home, away, far_here, far_there, cross_here, cross_there, *rows, *slots,
            ),
            [
                ((LANES, length), BF16),
                ((per_group, length, length), BF16),
                ((length, LANES), BF16),
                ((length, LANES), BF16),
                ((length, LANES), BF16),
                ((per_group, length, LANES), F32),
                ((LANES, model), BF16),
            ],
        )
        cums.append(part_cum)
    arrived = [slots[0]] + [sp_swap(slots[i], i) for i in range(1, split)]
    query_grad, key_grad, value_grad, cum_grad, grad_weight = call(
        functools.partial(place_kernel, split),
        [((tokens, attn), BF16)] * 3
        + [((heads, length), F32), ((block_rows, 2 * half), F32)],
        (*arrived, *cums, first, second, last, *parts),
    )
    return query_grad[None], key_grad[None], value_grad[None], cum_grad[None], grad_weight


def head_grads(query, keys, values, output, cotangent, cum):
    _, length, head_width = query.shape
    span_rows = min(512, length)
    score_scale = head_width ** (-0.5)
    row_dots = jnp.sum(cotangent.astype(jnp.float32) * output.astype(jnp.float32), axis=2)
    positions = jnp.arange(length)

    def product(left, right, form):
        return jnp.einsum(form, left, right, preferred_element_type=jnp.float32)

    def advance(totals, block_index):
        key_grad, value_grad, cum_grad = totals
        offset = block_index * span_rows
        query_blk = lax.dynamic_slice_in_dim(query, offset, span_rows, 1)
        cot_blk = lax.dynamic_slice_in_dim(cotangent, offset, span_rows, 1)
        cum_blk = lax.dynamic_slice_in_dim(cum, offset, span_rows, 1)
        dots_blk = lax.dynamic_slice_in_dim(row_dots, offset, span_rows, 1)
        scores = product(query_blk, keys, "hqe,hke->hqk") * score_scale
        scores = scores + cum_blk[:, :, None] - cum[:, None, :]
        query_pos = offset + jnp.arange(span_rows)
        causal = positions[None, :] <= query_pos[:, None]
        scores = jnp.where(causal[None], scores, -1e30)
        row_max = jnp.max(scores, axis=2, keepdims=True)
        weights = jnp.exp(scores - row_max)
        weights = weights / jnp.sum(weights, axis=2, keepdims=True)
        weights_b = weights.astype(jnp.bfloat16)
        d_prob = product(cot_blk, values, "hqe,hke->hqk")
        d_score = weights * (d_prob - dots_blk[:, :, None])
        score_b = d_score.astype(jnp.bfloat16)
        query_grad = (product(score_b, keys, "hqk,hke->hqe") * score_scale).astype(jnp.bfloat16)
        key_grad = key_grad + product(score_b, query_blk, "hqk,hqe->hke") * score_scale
        value_grad = value_grad + product(weights_b, cot_blk, "hqk,hqe->hke")
        cum_grad = cum_grad - jnp.sum(d_score, axis=1)
        own_part = lax.dynamic_slice_in_dim(cum_grad, offset, span_rows, 1) + jnp.sum(
            d_score, axis=2
        )
        cum_grad = lax.dynamic_update_slice_in_dim(cum_grad, own_part, offset, 1)
        return ((key_grad, value_grad, cum_grad), query_grad)

    start_state = (
        jnp.zeros(query.shape, jnp.float32),
        jnp.zeros(query.shape, jnp.float32),
        jnp.zeros(cum.shape, jnp.float32),
    )
    totals, query_blocks = lax.scan(advance, start_state, jnp.arange(length // span_rows))
    query_grad = jnp.transpose(query_blocks, (1, 0, 2, 3)).reshape(query.shape)
    return (query_grad, totals[0].astype(jnp.bfloat16), totals[1].astype(jnp.bfloat16), totals[2])


def shards(query, keys, values, output, cum, d_out, w_out):
    local_rows = d_out[0]
    whole_output = output[0]
    d_attn = lax.dot_general(
        local_rows,
        lax.all_gather(w_out, "dp", axis=0, tiled=True),
        (((1,), (1,)), ((), ())),
        preferred_element_type=jnp.float32,
    ).astype(jnp.bfloat16)
    head_cot, column_part = (
        lax.all_to_all(d_attn[None], "sp", split_axis=2, concat_axis=1, tiled=True),
        lax.all_to_all(d_out, "sp", split_axis=2, concat_axis=1, tiled=True),
    )
    grad_weight = lax.psum_scatter(
        lax.dot_general(
            whole_output,
            column_part[0],
            (((0,), (0,)), ((), ())),
            preferred_element_type=jnp.float32,
        ),
        "dp",
        scatter_dimension=0,
        tiled=True,
    )
    head_cols = query.shape[2]
    head_count = cum.shape[1]
    head_width = head_cols // head_count
    seq_length = query.shape[1]
    own_output = lax.dynamic_slice_in_dim(
        whole_output, lax.axis_index("sp") * head_cols, head_cols, 1
    )

    def heads_first(matrix):
        return jnp.transpose(matrix.reshape(seq_length, head_count, head_width), (1, 0, 2))

    def tokens_first(matrix):
        return jnp.transpose(matrix, (1, 0, 2)).reshape(1, seq_length, head_cols)

    grads = head_grads(
        heads_first(query[0]),
        heads_first(keys[0]),
        heads_first(values[0]),
        heads_first(own_output),
        heads_first(head_cot[0]),
        cum[0],
    )
    query_grad, key_grad, value_grad = (
        lax.all_to_all(tokens_first(grads[0]), "sp", split_axis=1, concat_axis=2, tiled=True),
        lax.all_to_all(tokens_first(grads[1]), "sp", split_axis=1, concat_axis=2, tiled=True),
        lax.all_to_all(tokens_first(grads[2]), "sp", split_axis=1, concat_axis=2, tiled=True),
    )
    return (query_grad, key_grad, value_grad, grads[3][None], grad_weight)


def fits(sizes, args):
    split, groups = sizes
    query, output, cum, d_out, w_out = args[0], args[3], args[4], args[5], args[6]
    _, attn = query.shape[1:]
    width, heads = attn // split, cum.shape[1] // split
    head_width = width // max(heads, 1)
    return (
        split == 4
        and groups == 2 * split
        and width == 2 * LANES
        and heads * head_width == width
        and LANES % head_width == 0
        and 8 % heads == 0
        and head_width**0.5 % 1 == 0
        and head_width & (head_width - 1) == 0
        and w_out.shape[0] // groups == LANES
        and output.shape[2] == attn
        and d_out.shape[1] // split == LANES
        and d_out.shape[2] % (split * LANES) == 0
    )


def solution(mesh):
    placed = (
        P("dp", None, "sp"),
        P("dp", None, "sp"),
        P("dp", None, "sp"),
        P("dp", None, None),
        P("dp", "sp", None),
        P("dp", "sp", None),
        P("dp", None),
    )
    sizes = (mesh.shape["sp"], mesh.shape["dp"])

    def step(*args):
        body = functools.partial(fused_shards, sizes) if fits(sizes, args) else shards
        return jax.shard_map(
            body,
            mesh=mesh,
            in_specs=placed,
            out_specs=(
                P("dp", "sp", None),
                P("dp", "sp", None),
                P("dp", "sp", None),
                P("dp", "sp", None),
                P("dp", "sp"),
            ),
            check_vma=False,
        )(*args)

    return step
```
